32 devices in a mesh: grp: 1, fs: 2 (over x), tp: 16 (over z, y, core).
Axes of the slice: x: 2, y: 2, z: 4, core: 2. Of those that a mesh axis runs over, the one named last changes fastest.
Arguments:
- prompt_rows: bfloat16 [512, 2048], P(('grp', 'fs')), may hold values from -6 to 6
- gain_before: float32 [2048], P('fs'), may hold values from 0.1 to 1.9
- gate_before: float32 [2048, 5632], P('fs', 'tp'), may hold values from -0.125 to 0.125
- up_before: float32 [2048, 5632], P('fs', 'tp'), may hold values from -0.125 to 0.125
- down_before: float32 [5632, 2048], P('fs', 'tp'), may hold values from -0.3125 to 0.3125
- gain_after: float32 [2048], P('fs'), may hold values from 0.1 to 1.9
- gate_after: float32 [2048, 5632], P('fs', 'tp'), may hold values from -0.125 to 0.125
- up_after: float32 [2048, 5632], P('fs', 'tp'), may hold values from -0.125 to 0.125
- down_after: float32 [5632, 2048], P('fs', 'tp'), may hold values from -0.3125 to 0.3125
Outputs:
- mixed_rows: bfloat16 [512, 2048], P(('grp', 'fs'))
- served_gate_before: bfloat16 [2048, 5632], P('grp', 'tp')
- served_up_before: bfloat16 [2048, 5632], P('grp', 'tp')
- served_down_before: bfloat16 [5632, 2048], P(('grp', 'tp'))
- served_gate_after: bfloat16 [2048, 5632], P('grp', 'tp')
- served_up_after: bfloat16 [2048, 5632], P('grp', 'tp')
- served_down_after: bfloat16 [5632, 2048], P(('grp', 'tp'))
The draws below stay inside these ranges and needn't reach their ends.
All inputs are finite; a program needn't handle non-finite values.
Results may differ from the reference program's by a relative error of at most 0.03.
Values may be sent and summed in bfloat16 or wider, within the bound.
No kernel may reach another device: no remote copies, remote signals or barrier semaphores. Data moves between devices by JAX's collectives and lax.ppermute only.
A program may use at most 64 MiB of HBM per device.

```python
import jax
import jax.numpy as jnp
from jax import lax

D = 2048
FF = 5632
TOKENS = 512
N_TP = 16


def levels(own_key, extent, cuts, least, largest):
    level, own = 1.0, jax.random.fold_in(own_key, 6)
    for position, shards_of in cuts:
        draws = jnp.exp(jax.random.uniform(jax.random.fold_in(own, position), (shards_of,), jnp.float32, least / len(cuts), largest / len(cuts)))
        level = level * jnp.repeat(draws, extent[position] // shards_of).reshape([-1 if axis == position else 1 for axis in range(len(extent))])
    return level


def scatter_about(rng, extent, spread, bound, pieces=(), kind=jnp.bfloat16):
    entries = spread * jax.random.normal(rng, extent, jnp.float32)
    if pieces:
        entries = entries * levels(rng, extent, pieces, -0.22, 0.18)
    return jnp.clip(entries, -bound, bound).astype(kind)


def setup_inputs(seed: int = 0, part: int = 0) -> dict:
    key_list = jax.random.split(jax.random.key(seed), 10)
    part_splits = jax.random.split(jax.random.fold_in(key_list[9], part), 10)
    return {
        "prompt_rows": scatter_about(part_splits[0], (TOKENS, D), 1.0, 6.0, ((0, 2),)),
        "gain_before": jnp.clip(1.0 + 0.18 * jax.random.normal(key_list[1], (D,), jnp.float32), 0.1, 1.9),
        "gate_before": scatter_about(key_list[2], (D, FF), D ** -0.5, 0.125, ((0, 2), (1, 16)), jnp.float32),
        "up_before": scatter_about(key_list[3], (D, FF), D ** -0.5, 0.125, ((0, 2), (1, 16)), jnp.float32),
        "down_before": scatter_about(key_list[4], (FF, D), (FF // 16) ** -0.5, 0.3125, ((0, 2), (1, 16)), jnp.float32),
        "gain_after": jnp.clip(1.0 + 0.18 * jax.random.normal(key_list[5], (D,), jnp.float32), 0.1, 1.9),
        "gate_after": scatter_about(key_list[6], (D, FF), D ** -0.5, 0.125, ((0, 2), (1, 16)), jnp.float32),
        "up_after": scatter_about(key_list[7], (D, FF), D ** -0.5, 0.125, ((0, 2), (1, 16)), jnp.float32),
        "down_after": scatter_about(key_list[8], (FF, D), (FF // 16) ** -0.5, 0.3125, ((0, 2), (1, 16)), jnp.float32),
    }


EPS = 1e-06

def fold(gain, gate_w, up_w, down_w):
    served_gate = (gain[:, None] * gate_w).astype(jnp.bfloat16)
    served_up = (gain[:, None] * up_w).astype(jnp.bfloat16)
    return (served_gate, served_up, down_w.astype(jnp.bfloat16))

def half_step(row_block, gate_w, up_w, down_w):
    values = row_block.astype(jnp.float32)
    normed = (values * lax.rsqrt(lax.optimization_barrier(jnp.mean(values * values, axis=-1, keepdims=True)) + EPS)).astype(jnp.bfloat16)
    gate_pre = jnp.dot(normed, gate_w, preferred_element_type=jnp.float32)
    up_pre = jnp.dot(normed, up_w, preferred_element_type=jnp.float32)
    hidden = (jax.nn.silu(gate_pre) * up_pre).astype(jnp.bfloat16)
    width = FF // N_TP
    hidden_blocks = hidden.reshape(hidden.shape[0], N_TP, width).transpose(1, 0, 2)
    down_blocks = down_w.reshape(N_TP, width, D)

    def add_block(total, pair):
        part_sum = jnp.dot(pair[0], pair[1], preferred_element_type=jnp.float32).astype(jnp.bfloat16)
        part_sum = lax.optimization_barrier(part_sum)
        return (total + part_sum.astype(jnp.float32), None)
    total, _ = lax.scan(add_block, jnp.zeros((hidden.shape[0], D), jnp.float32), (hidden_blocks, down_blocks))
    return (values + 0.5 * total).astype(jnp.bfloat16)

def reference(prompt_rows, gain_before, gate_before, up_before, down_before, gain_after, gate_after, up_after, down_after):
    gate_one, up_one, down_one = fold(gain_before, gate_before, up_before, down_before)
    gate_two, up_two, down_two = fold(gain_after, gate_after, up_after, down_after)
    middle = half_step(prompt_rows, gate_one, up_one, down_one)
    mixed = half_step(middle, gate_two, up_two, down_two)
    return (mixed, gate_one, up_one, down_one, gate_two, up_two, down_two)
```

```python
import jax
import jax.numpy as jnp
from jax import lax
from jax.sharding import PartitionSpec as P


EPS = 1e-06


def swap_fs(value, n_fs):
    return lax.ppermute(value, "fs", [(i, i ^ 1) for i in range(n_fs)])


def stack_fs(value, n_fs):
    if n_fs == 2:
        other = swap_fs(value, n_fs)
        first = lax.axis_index("fs") == 0
        return jnp.concatenate(
            [jnp.where(first, value, other), jnp.where(first, other, value)], axis=0
        )
    return lax.all_gather(value, "fs", axis=0, tiled=True)


def serve_down(down_w, n_fs, n_tp):
    down_half = down_w.astype(jnp.bfloat16)
    if n_fs != 2 or (down_w.shape[0] // n_tp) % 8:
        tall_block = lax.all_gather(down_half, "fs", axis=0, tiled=True)
        return lax.all_to_all(tall_block, "tp", split_axis=0, concat_axis=1, tiled=True)
    rows, width = down_w.shape[0] // n_tp, down_w.shape[1]
    parts = down_half.reshape(n_tp // 2, 2, rows, width)
    place = lax.axis_index("fs")
    keep = lax.dynamic_index_in_dim(parts, place, 1, keepdims=False)
    send = lax.dynamic_index_in_dim(parts, 1 - place, 1, keepdims=False)
    other = swap_fs(send, n_fs)
    first = place == 0
    tall = jnp.concatenate(
        [jnp.where(first, keep, other), jnp.where(first, other, keep)], axis=0
    )
    got = lax.all_to_all(tall, "tp", 0, 0, tiled=True)
    band = got.transpose(1, 0, 2).reshape(rows, n_tp * width)
    return stack_fs(band, n_fs)


def serve_weight(gain, weight, n_fs):
    half = (gain[:, None] * weight).astype(jnp.bfloat16)
    return stack_fs(half, n_fs)


def pair_swap(value, n_tp):
    return lax.ppermute(value, "tp", [(i, i ^ 1) for i in range(n_tp)])


def swap_places(value, n_tp, mask):
    return lax.ppermute(value, "tp", [(i, i ^ (2 * mask)) for i in range(n_tp)])


def scatter_sum(part, n_tp):
    rows, width = part.shape
    core, place = lax.axis_index("tp") % 2, lax.axis_index("tp") // 2
    places = n_tp // 2
    halves = part.reshape(2, rows // 2, width)
    keep = lax.dynamic_index_in_dim(halves, core, 0, keepdims=False)
    send = lax.dynamic_index_in_dim(halves, 1 - core, 0, keepdims=False)
    other = pair_swap(send, n_tp)
    both = keep.astype(jnp.float32) + other.astype(jnp.float32)
    bands = both.astype(jnp.bfloat16).reshape(places, rows // n_tp, width)
    got = [
        swap_places(lax.dynamic_index_in_dim(bands, place ^ mask, 0, keepdims=False), n_tp, mask)
        for mask in range(1, places)
    ]
    total = lax.dynamic_index_in_dim(bands, place, 0, keepdims=False).astype(jnp.float32)
    for piece in got:
        total = total + piece.astype(jnp.float32)
    return total


def my_band(rows_block, n_tp):
    rows = rows_block.shape[0] // n_tp
    index = lax.axis_index("tp")
    band = (index % 2) * (n_tp // 2) + index // 2
    return lax.dynamic_slice_in_dim(rows_block, band * rows, rows, axis=0)


def gather_bands(band, n_tp):
    place, places = lax.axis_index("tp") // 2, n_tp // 2
    got = [band] + [swap_places(band, n_tp, mask) for mask in range(1, places)]
    half = jnp.zeros((places,) + band.shape, band.dtype)
    for mask, piece in enumerate(got):
        half = lax.dynamic_update_index_in_dim(half, piece, place ^ mask, 0)
    half = half.reshape(-1, band.shape[1])
    other = pair_swap(half, n_tp)
    first = lax.axis_index("tp") % 2 == 0
    return jnp.concatenate([jnp.where(first, half, other), jnp.where(first, other, half)], axis=0)


def normalise(values):
    return (values * lax.rsqrt(jnp.mean(values * values, axis=-1, keepdims=True) + EPS)).astype(
        jnp.bfloat16
    )


def part_of(normed, gate_w, up_w, down_w):
    gate_pre = jnp.dot(normed, gate_w, preferred_element_type=jnp.float32)
    up_pre = jnp.dot(normed, up_w, preferred_element_type=jnp.float32)
    hidden = (jax.nn.silu(gate_pre) * up_pre).astype(jnp.bfloat16)
    return jnp.dot(hidden, down_w, preferred_element_type=jnp.float32).astype(jnp.bfloat16)


def make_body(n_fs, n_tp):
    def body(
        prompt_rows,
        gain_before,
        gate_before,
        up_before,
        down_before,
        gain_after,
        gate_after,
        up_after,
        down_after,
    ):
      one = (
          serve_weight(gain_before, gate_before, n_fs),
          serve_weight(gain_before, up_before, n_fs),
          serve_down(down_before, n_fs, n_tp),
      )
      two = (
          serve_weight(gain_after, gate_after, n_fs),
          serve_weight(gain_after, up_after, n_fs),
          serve_down(down_after, n_fs, n_tp),
      )
      normed = normalise(prompt_rows.astype(jnp.float32))
      band = my_band(prompt_rows, n_tp).astype(jnp.float32)
      total = scatter_sum(part_of(normed, *one), n_tp)
      middle = (band + 0.5 * total).astype(jnp.bfloat16).astype(jnp.float32)
      normed = gather_bands(normalise(middle), n_tp)
      total = scatter_sum(part_of(normed, *two), n_tp)
      mixed = gather_bands((middle + 0.5 * total).astype(jnp.bfloat16), n_tp)
      return (mixed,) + one + two

    return body


def solution(mesh):
    placed = (
        P(("grp", "fs"), None),
        P("fs"),
        P("fs", "tp"),
        P("fs", "tp"),
        P("fs", "tp"),
        P("fs"),
        P("fs", "tp"),
        P("fs", "tp"),
        P("fs", "tp"),
    )
    return jax.shard_map(
        make_body(mesh.shape["fs"], mesh.shape["tp"]),
        mesh=mesh,
        in_specs=placed,
        out_specs=(
            P(("grp", "fs"), None),
            P("grp", "tp"),
            P("grp", "tp"),
            P(("grp", "tp"), None),
            P("grp", "tp"),
            P("grp", "tp"),
            P(("grp", "tp"), None),
        ),
        check_vma=False,
    )
```
